32 devices in a mesh: sp: 16 (over z, y, x), tp: 2 (over core).
Axes of the slice: x: 2, y: 2, z: 4, core: 2. Of those that a mesh axis runs over, the one named last changes fastest.
Arguments:
- tokens: bfloat16 [12288, 2048], P(('sp', 'tp')), may hold values from -6 to 6
- input_gain: float32 [2048], replicated, may hold values from 0.1 to 1.9
- branch_value: bfloat16 [2048, 1024], P('sp', 'tp'), may hold values from -0.125 to 0.125
- branch_gate: bfloat16 [2048, 1024], P('sp', 'tp'), may hold values from -0.125 to 0.125
- query_weight: bfloat16 [2048, 1024], P('sp', 'tp'), may hold values from -0.125 to 0.125
- key_weight: bfloat16 [2048, 1024], P('sp', 'tp'), may hold values from -0.125 to 0.125
- value_weight: bfloat16 [2048, 1024], P('sp', 'tp'), may hold values from -0.125 to 0.125
- swish_weight: bfloat16 [2048, 1024], P('sp', 'tp'), may hold values from -0.125 to 0.125
- kernel_taps: float32 [31, 1024], P(None, 'tp'), may hold values from -8 to 8
- channel_gain: float32 [1024], P('tp'), may hold values from 0.1 to 1.9
- decay_logs: float32 [16, 12288], P('tp', 'sp'), may hold values from -1.5 to 0
- start_state: float32 [2, 16, 64, 64], P(None, 'tp')
- head_gain: float32 [1024], P('tp'), may hold values from 0.1 to 1.9
- output_conv: bfloat16 [1024, 2048], P('tp', 'sp'), may hold values from -0.125 to 0.125
- output_heads: bfloat16 [1024, 2048], P('tp', 'sp'), may hold values from -0.125 to 0.125
Outputs:
- mixed: bfloat16 [12288, 2048], P(('sp', 'tp'))
The draws below stay inside these ranges and needn't reach their ends.
All inputs are finite; a program needn't handle non-finite values.
Results may differ from the reference program's by a relative error of at most 0.018.
Values may be sent and summed in bfloat16 or wider, within the bound.
A program may use at most 64 MiB of HBM per device.

```python
import math
import jax
import jax.numpy as jnp
from jax import lax

D = 2048
DC = 1024
HEADS = 16
HD = 64
TAPS = 31
BLOCK = 256
TOKENS = 12288
N_TP = 2


def draw_kernel_taps(key, part):
    first_key = jax.random.fold_in(key, 0)
    ramp = jnp.exp(math.log(10.0) * jnp.arange(DC, dtype=jnp.float32) / (DC - 1))
    base = jnp.clip(jax.random.normal(first_key, (TAPS, DC), jnp.float32), -4.0, 4.0)
    return base * ramp[None, :] / math.sqrt(TAPS)


def draw_decay_logs(key, part):
    subkeys = jax.random.split(key, 6)
    ranking = jax.random.permutation(subkeys[0], HEADS)
    fast_count = HEADS // 2
    fast_mask = ranking < fast_count
    fast_rate = jnp.exp(jax.random.uniform(subkeys[1], (HEADS,), jnp.float32, math.log(0.01), math.log(1.0 / 30.0)))
    slow_rate = jnp.exp(jax.random.uniform(subkeys[2], (HEADS,), jnp.float32, math.log(0.15), math.log(0.4))) / TOKENS
    base_rate = jnp.where(fast_mask, fast_rate, slow_rate)
    block_count = TOKENS // BLOCK
    factor = jnp.exp(jax.random.uniform(subkeys[3], (HEADS, block_count), jnp.float32, math.log(0.5), math.log(2.0)))
    decay_factors = jnp.repeat(base_rate[:, None] * factor, BLOCK, axis=1)
    segment_locations = jax.random.randint(subkeys[4], (HEADS, 2), 0, TOKENS)
    decay_amounts = jnp.log(jax.random.uniform(subkeys[5], (HEADS, 2), jnp.float32, 0.5, 0.8))
    token_positions = jnp.arange(TOKENS, dtype=jnp.int32)
    token_segments = jnp.sum(jnp.where(token_positions[None, None, :] == segment_locations[:, :, None], decay_amounts[:, :, None], 0.0), axis=1)
    return token_segments - decay_factors


def draw_start_state(key, part):
    magnitude = math.sqrt(TOKENS) / 4.0
    base = jnp.clip(jax.random.normal(key, (2, HEADS, HD, HD), jnp.float32), -4.0, 4.0)
    return base * magnitude


def shard_levels(rng, extent, cuts, least, largest):
    factor_of = 1.0
    for position, shards_of in cuts:
        draws = jax.random.uniform(jax.random.fold_in(jax.random.fold_in(rng, 6), position), (shards_of,), jnp.float32, least / len(cuts), largest / len(cuts))
        factor_of = factor_of * jnp.repeat(jnp.exp(draws), extent[position] // shards_of).reshape((-1,) + (1,) * (len(extent) - 1 - position))
    return factor_of


def scatter_about(own_key, extent, scale, limit, shards=(), kind=jnp.bfloat16):
    gain = shard_levels(own_key, extent, shards, -0.22, 0.18) if shards else 1.0
    values = jax.random.normal(own_key, extent, jnp.float32) * scale * gain
    return jnp.minimum(jnp.maximum(values, -limit), limit).astype(kind)


def setup_inputs(seed: int = 0) -> dict:
    key_list = jax.random.split(jax.random.key(seed), 16)
    tokens = scatter_about(key_list[0], (TOKENS, D), 1.0, 6.0, ((0, 32),))
    input_gain = jnp.clip(1.0 + 0.18 * jax.random.normal(key_list[1], (D,), jnp.float32), 0.1, 1.9)
    branch_value = scatter_about(key_list[2], (D, DC), D ** -0.5, 0.125, ((0, 16), (1, 2)))
    branch_gate = scatter_about(key_list[3], (D, DC), D ** -0.5, 0.125, ((0, 16), (1, 2)))
    query_weight = scatter_about(key_list[4], (D, HEADS * HD), D ** -0.5, 0.125, ((0, 16), (1, 2)))
    key_weight = scatter_about(key_list[5], (D, HEADS * HD), D ** -0.5, 0.125, ((0, 16), (1, 2)))
    value_weight = scatter_about(key_list[6], (D, HEADS * HD), D ** -0.5, 0.125, ((0, 16), (1, 2)))
    swish_weight = scatter_about(key_list[7], (D, HEADS * HD), D ** -0.5, 0.125, ((0, 16), (1, 2)))
    kernel_taps = draw_kernel_taps(jax.random.fold_in(key_list[15], 71), 0)
    channel_gain = jnp.clip(1.0 + 0.18 * jax.random.normal(key_list[9], (DC,), jnp.float32), 0.1, 1.9)
    decay_logs = draw_decay_logs(jax.random.fold_in(key_list[15], 71), 0)
    start_state = draw_start_state(jax.random.fold_in(key_list[15], 71), 0)
    head_gain = jnp.clip(1.0 + 0.18 * jax.random.normal(key_list[12], (HEADS * HD,), jnp.float32), 0.1, 1.9)
    output_conv = scatter_about(key_list[13], (DC, D), (DC + HEADS * HD) ** -0.5, 0.125, ((0, 2), (1, 16)))
    output_heads = scatter_about(key_list[14], (HEADS * HD, D), (DC + HEADS * HD) ** -0.5, 0.125, ((0, 2), (1, 16)))
    return dict(tokens=tokens, input_gain=input_gain, branch_value=branch_value, branch_gate=branch_gate, query_weight=query_weight, key_weight=key_weight, value_weight=value_weight, swish_weight=swish_weight, kernel_taps=kernel_taps, channel_gain=channel_gain, decay_logs=decay_logs, start_state=start_state, head_gain=head_gain, output_conv=output_conv, output_heads=output_heads)


EPSILON = 1e-06
HIGHEST = lax.Precision.HIGHEST

def block_states(scaled_keys, values_block, running):
    closing = running[:, :, -1:]
    totals = jnp.exp(closing[:, :, 0])
    toward_end = jnp.exp(closing - running).transpose(0, 2, 1)[:, :, :, None]
    from_start = jnp.exp(running).transpose(0, 2, 1)[:, :, :, None]
    forward = jnp.einsum('nshd,nshe->nhde', scaled_keys * toward_end, values_block, precision=HIGHEST)
    backward = jnp.einsum('nshd,nshe->nhde', scaled_keys * from_start, values_block, precision=HIGHEST)
    return (totals, forward, backward)

def block_outputs(queries, scaled_keys, values_block, running, forward_in, backward_in):
    length = queries.shape[1]
    scores = jnp.einsum('nthd,nshd->nhts', queries, scaled_keys, precision=HIGHEST)
    distance = jnp.abs(running[:, :, :, None] - running[:, :, None, :])
    weights = jnp.exp(-distance) + jnp.eye(length, dtype=jnp.float32)
    within = jnp.einsum('nhts,nshe->nthe', scores * weights, values_block, precision=HIGHEST)
    from_start = jnp.exp(running).transpose(0, 2, 1)[:, :, :, None]
    toward_end = jnp.exp(running[:, :, -1:] - running).transpose(0, 2, 1)[:, :, :, None]
    earlier = jnp.einsum('nthd,nhde->nthe', queries, forward_in, precision=HIGHEST)
    after_part = jnp.einsum('nthd,nhde->nthe', queries, backward_in, precision=HIGHEST)
    return within + from_start * earlier + toward_end * after_part

def head_output(retained, gates_in, head_gain):
    row_count = retained.shape[0]
    centred = retained - lax.optimization_barrier(jnp.mean(retained, axis=2, keepdims=True))
    scaled = centred * lax.rsqrt(lax.optimization_barrier(jnp.mean(centred * centred, axis=2, keepdims=True)) + EPSILON)
    flattened = scaled.reshape(row_count, -1) * head_gain[None, :]
    return (flattened * jax.nn.silu(gates_in.astype(jnp.float32))).astype(jnp.bfloat16)

def reference(tokens, input_gain, branch_value, branch_gate, query_weight, key_weight, value_weight, swish_weight, kernel_taps, channel_gain, decay_logs, start_state, head_gain, output_conv, output_heads):
    widened = tokens.astype(jnp.float32)
    inverse = lax.rsqrt(lax.optimization_barrier(jnp.mean(widened * widened, axis=1, keepdims=True)) + EPSILON)
    normed = (widened * inverse * input_gain[None, :]).astype(jnp.bfloat16)

    def project(weight):
        return jnp.dot(normed, weight, preferred_element_type=jnp.float32)
    gated_rows = (project(branch_value) * jax.nn.sigmoid(project(branch_gate))).astype(jnp.bfloat16)
    queries_in = project(query_weight).astype(jnp.bfloat16)
    keys_in = project(key_weight).astype(jnp.bfloat16)
    values_in = project(value_weight).astype(jnp.bfloat16)
    gates_in = project(swish_weight).astype(jnp.bfloat16)
    half_width = TAPS // 2
    padded = jnp.pad(gated_rows.astype(jnp.float32), ((half_width, half_width), (0, 0)))
    convolved = jnp.zeros((TOKENS, DC), jnp.float32)
    for offset in range(TAPS):
        convolved = convolved + kernel_taps[offset][None, :] * padded[offset:offset + TOKENS]
    average = lax.optimization_barrier(jnp.mean(convolved, axis=1, keepdims=True))
    squares = lax.optimization_barrier(jnp.mean(convolved * convolved, axis=1, keepdims=True))
    normalized = (convolved - average) * lax.rsqrt(squares - average * average + EPSILON)
    branch_out = jax.nn.silu(normalized * channel_gain[None, :]).astype(jnp.bfloat16)
    blocks = TOKENS // BLOCK

    def split_heads(matrix):
        return matrix.astype(jnp.float32).reshape(blocks, BLOCK, HEADS, HD)
    query_blocks = split_heads(queries_in)
    key_blocks = split_heads(keys_in) * HD ** (-0.5)
    value_blocks = split_heads(values_in)
    running = jnp.cumsum(decay_logs.reshape(HEADS, blocks, BLOCK).transpose(1, 0, 2), axis=2)
    totals, forward, backward = block_states(key_blocks, value_blocks, running)

    def carry_step(carried, member):
        return (member[0][:, None, None] * carried + member[1], carried)
    final_forward, forward_in = lax.scan(carry_step, start_state[0], (totals, forward))
    final_backward, backward_in = lax.scan(carry_step, start_state[1], (totals, backward), reverse=True)

    def one_block(member):
        result = block_outputs(member[0][None], member[1][None], member[2][None], member[3][None], member[4][None], member[5][None])
        return result[0]
    retained = lax.map(one_block, (query_blocks, key_blocks, value_blocks, running, forward_in, backward_in))
    retained = retained.reshape(TOKENS, HEADS, HD)
    heads_out = head_output(retained, gates_in, head_gain)
    conv_group = DC // N_TP
    head_group = HEADS * HD // N_TP
    summed = jnp.zeros((TOKENS, D), jnp.float32)
    for group_index in range(N_TP):
        conv_slice = slice(group_index * conv_group, (group_index + 1) * conv_group)
        head_slice = slice(group_index * head_group, (group_index + 1) * head_group)
        partial_sum = jnp.dot(branch_out[:, conv_slice], output_conv[conv_slice], preferred_element_type=jnp.float32)
        partial_sum = partial_sum + jnp.dot(heads_out[:, head_slice], output_heads[head_slice], preferred_element_type=jnp.float32)
        rounded = lax.optimization_barrier(partial_sum.astype(jnp.bfloat16))
        summed = summed + rounded.astype(jnp.float32)
    return summed.astype(jnp.bfloat16)
```

```python
import functools
import jax
import jax.numpy as jnp
from jax import lax
from jax.experimental import pallas as pl
from jax.experimental.pallas import tpu as pltpu
from jax.sharding import PartitionSpec as P

DC = 1024
HD = 64
BLOCK = 256
SIDE = 2
MESH_ID = pl.DeviceIdType.MESH


class Router:
    def __init__(self, count, unit):
        self.depth = count // (SIDE * SIDE)
        me = lax.axis_index("sp")
        self.x = lax.rem(me, SIDE)
        self.y = lax.rem(me // SIDE, SIDE)
        self.z = me // (SIDE * SIDE)
        self.routes = (
            ("zxy", 0, 3 * unit),
            ("zyx", 3 * unit, 3 * unit),
            ("xyz", 6 * unit, unit),
            ("yxz", 7 * unit, unit),
        )
        reach = [(0, None)]
        for d in range(1, self.depth):
            reach += [(-d, self.z - d >= 0), (d, self.z + d < self.depth)]
        self.events = []
        for dz, valid in reach:
            for dy in range(SIDE):
                for dx in range(SIDE):
                    if dz == dy == dx == 0:
                        continue
                    for r, (order, _, _) in enumerate(self.routes):
                        self.events.append((abs(dz) + dy + dx, r, dz, dy, dx, valid))
        self.events.sort(key=lambda e: (e[0], e[1], e[2], e[3], e[4]))

    def index(self, z, y, x):
        return (z * SIDE + y) * SIDE + x

    def source(self, dz, dy, dx):
        y = self.y if dy == 0 else 1 - self.y
        x = self.x if dx == 0 else 1 - self.x
        return self.index(self.z + dz, y, x)

    def neighbours(self):
        z, y, x = self.z, self.y, self.x
        return {
            "x": (self.index(z, y, 1 - x), None),
            "y": (self.index(z, 1 - y, x), None),
            "+": (self.index(z + 1, y, x), z + 1 < self.depth),
            "-": (self.index(z - 1, y, x), z - 1 >= 0),
        }

    def targets(self, r, dz, dy, dx):
        order = self.routes[r][0]
        off = {"z": dz, "y": dy, "x": dx}
        last = max([i for i, d in enumerate(order) if off[d] != 0], default=-1)
        out = []
        if last >= 0 and order[last] == "z":
            out.append("+" if dz < 0 else "-")
        for d in order[last + 1 :]:
            out += ["+", "-"] if d == "z" else [d]
        return out


def when(cond, fn):
    if cond is None:
        fn()
    else:
        pl.when(cond)(fn)


def both(a, b):
    if a is None:
        return b
    if b is None:
        return a
    return jnp.logical_and(a, b)


DIRECTIONS = "xy+-"


def enter(router, partner):
    barrier = pltpu.get_barrier_semaphore()
    near = router.neighbours()
    for idx, valid in near.values():

        def greet(idx=idx):
            pl.semaphore_signal(barrier, inc=1, device_id={"sp": idx}, device_id_type=MESH_ID)

        when(valid, greet)
    extra = 0
    if partner is not None:
        pl.semaphore_signal(barrier, inc=1, device_id={"tp": partner}, device_id_type=MESH_ID)
        extra = 1
    ends = sum(jnp.where(near[d][1], 1, 0) for d in "+-")
    pl.semaphore_wait(barrier, 2 + extra + ends)


class Flow:
    def __init__(self, router, local, gathered, rows, send_sem, recv_sem):
        self.router, self.local, self.gathered, self.rows = router, local, gathered, rows
        self.send_sem, self.recv_sem = send_sem, recv_sem

    def copy(self, g, r, dz, dy, dx, d):
        router = self.router
        _, first, count = router.routes[r]
        s = router.source(dz, dy, dx)
        place = self.gathered.at[g, s, pl.ds(first, count), :]
        src = self.local.at[g, pl.ds(first, count), :] if dz == dy == dx == 0 else place
        idx, valid = router.neighbours()[d]
        k = DIRECTIONS.index(d)
        return (
            pltpu.make_async_remote_copy(
                src_ref=src,
                dst_ref=place,
                send_sem=self.send_sem.at[g, r, k, s],
                recv_sem=self.recv_sem.at[g, r, s],
                device_id={"sp": idx},
                device_id_type=MESH_ID,
            ),
            valid,
        )

    def send(self, g, r, dz, dy, dx, wait=False):
        for d in self.router.targets(r, dz, dy, dx):
            copy, valid = self.copy(g, r, dz, dy, dx, d)
            when(valid, copy.wait_send if wait else copy.start)

    def own(self, g, wait=False):
        for r in range(len(self.router.routes)):
            self.send(g, r, 0, 0, 0, wait)

    def event(self, g, e):
        _, r, dz, dy, dx, cond = e

        def arrived():
            self.copy(g, r, dz, dy, dx, "x")[0].wait_recv()
            self.send(g, r, dz, dy, dx)

        when(cond, arrived)

    def finish(self, g):
        self.own(g, True)
        for e in self.router.events:
            _, r, dz, dy, dx, cond = e
            if self.router.targets(r, dz, dy, dx):
                when(cond, functools.partial(self.send, g, r, dz, dy, dx, True))


def project_kernel(
    count, tokens, gain, local, gated_out, packed_out, last_out,
    gathered, raw, normed, send_sem, recv_sem, local_sem, swap_sem,
):
    groups, rows, width = local.shape
    router = Router(count, rows // 8)
    core = lax.axis_index("tp")
    partner = 1 - core
    own_rows = tokens.shape[0]
    flow = Flow(router, local, gathered, rows, send_sem, recv_sem)
    mine = pl.ds(pl.multiple_of(core * own_rows, own_rows), own_rows)
    me = lax.axis_index("sp")
    enter(router, partner)
    flow.own(0)
    swap = pltpu.make_async_remote_copy(
        src_ref=tokens, dst_ref=raw.at[mine, :], send_sem=swap_sem.at[0], recv_sem=swap_sem.at[1],
        device_id={"tp": partner}, device_id_type=MESH_ID,
    )
    swap.start()
    keep = pltpu.make_async_copy(tokens, raw.at[mine, :], local_sem.at[groups])
    keep.start()
    for g in range(groups):
        pltpu.make_async_copy(local.at[g], gathered.at[g, me], local_sem.at[g]).start()
    for g in range(groups):
        pltpu.make_async_copy(local.at[g], gathered.at[g, me], local_sem.at[g]).wait()
    keep.wait()
    swap.wait()
    n_events = len(router.events)
    half = normed.shape[0] // 2
    tiles = width // 256
    units = 2 * tiles
    norm_rows = normed.shape[0] // units

    def unit(it, u):
        @pl.when(it == 0)
        def _():
            window = pl.ds(u * norm_rows, norm_rows)
            widened = raw[window, :].astype(jnp.float32)
            inverse = lax.rsqrt(jnp.mean(widened * widened, axis=1, keepdims=True) + EPSILON)
            normed[window, :] = (widened * inverse * gain[...]).astype(jnp.bfloat16)

        @pl.when(it > 0)
        def _():
            m, n = u % 2, u // 2
            window = pl.ds(m * half, half)
            weight = gathered[it - 1, :, :, n * 256 : (n + 1) * 256].reshape(count * rows, 256)
            product = jnp.dot(normed[window, :], weight, preferred_element_type=jnp.float32)

            @pl.when(it == 1)
            def _():
                gated_out[window, n * 128 : (n + 1) * 128] = (
                    product[:, :128] * jax.nn.sigmoid(product[:, 128:])
                ).astype(jnp.bfloat16)

            @pl.when(it > 1)
            def _():
                column = pl.multiple_of((it - 2) * width + n * 256, 256)
                packed_out[window, pl.ds(column, 256)] = product.astype(jnp.bfloat16)

    def step(it, _):
        @pl.when(it < groups - 1)
        def _():
            flow.own(it + 1)

        done = 0
        for i, e in enumerate(router.events):
            flow.event(it, e)
            while done < units and (i + 1) * units >= (done + 1) * n_events:
                unit(it, done)
                done += 1
        return 0

    lax.fori_loop(0, groups, step, 0)
    out = pltpu.make_async_copy(gathered.at[groups - 1], last_out, local_sem.at[0])
    out.start()

    def drain(g, _):
        flow.finish(g)
        return 0

    lax.fori_loop(0, groups, drain, 0)
    out.wait()


def project(count, tokens, gain, local):
    groups, rows, width = local.shape
    total = tokens.shape[0] * 2
    model = tokens.shape[1]
    vmem = pl.BlockSpec(memory_space=pltpu.VMEM)
    return pl.pallas_call(
        functools.partial(project_kernel, count),
        out_shape=(
            jax.ShapeDtypeStruct((total, width // 2), jnp.bfloat16),
            jax.ShapeDtypeStruct((total, (groups - 2) * width), jnp.bfloat16),
            jax.ShapeDtypeStruct((count, rows, width), jnp.bfloat16),
        ),
        in_specs=[vmem] * 3,
        out_specs=(vmem, vmem, pl.BlockSpec(memory_space=pl.ANY)),
        scratch_shapes=[
            pltpu.VMEM((groups, count, rows, width), jnp.bfloat16),
            pltpu.VMEM((total, model), jnp.bfloat16),
            pltpu.VMEM((total, model), jnp.bfloat16),
            pltpu.SemaphoreType.DMA((groups, 4, 4, count)),
            pltpu.SemaphoreType.DMA((groups, 4, count)),
            pltpu.SemaphoreType.DMA((groups + 1,)),
            pltpu.SemaphoreType.DMA((2,)),
        ],
        compiler_params=pltpu.CompilerParams(
            collective_id=0, has_side_effects=True, vmem_limit_bytes=60 * 1024 * 1024
        ),
        name="project",
    )(tokens, gain.reshape(1, -1), local)


def gather_kernel(count, local, gathered, send_sem, recv_sem, local_sem):
    _, rows, _ = local.shape
    router = Router(count, rows // 8)
    flow = Flow(router, local, gathered, rows, send_sem, recv_sem)
    enter(router, None)
    flow.own(0)
    keep = pltpu.make_async_copy(local.at[0], gathered.at[0, lax.axis_index("sp")], local_sem.at[0])
    keep.start()
    for e in router.events:
        flow.event(0, e)
    keep.wait()
    flow.finish(0)


def gather_small(count, local):
    rows, width = local.shape
    vmem = pl.BlockSpec(memory_space=pltpu.VMEM)
    return pl.pallas_call(
        functools.partial(gather_kernel, count),
        out_shape=jax.ShapeDtypeStruct((1, count, rows, width), local.dtype),
        in_specs=[vmem],
        out_specs=vmem,
        scratch_shapes=[
            pltpu.SemaphoreType.DMA((1, 4, 4, count)),
            pltpu.SemaphoreType.DMA((1, 4, count)),
            pltpu.SemaphoreType.DMA((1,)),
        ],
        compiler_params=pltpu.CompilerParams(collective_id=1, has_side_effects=True),
        name="gather_states",
    )(local[None])[0]


EPSILON = 1e-06
HIGHEST = lax.Precision.HIGHEST


def with_halo(x, sides, width):
    for axis, dim in sides:
        count, length = (lax.axis_size(axis), x.shape[dim])
        up = [(i, (i + 1) % count) for i in range(count - 1)]
        down = [(j, i) for i, j in up]
        last = lax.slice_in_dim(x, length - width, length, axis=dim)
        first = lax.slice_in_dim(x, 0, width, axis=dim)
        before = lax.ppermute(last, axis, up)
        after = lax.ppermute(first, axis, down)
        x = jnp.concatenate([before, x, after], axis=dim)
    return x


def prefix(x, axis, join, neutral, backward):
    count = lax.axis_size(axis)
    place = lax.axis_index(axis)
    ahead = count - 1 - place if backward else place
    gathered = jax.tree.map(
        lambda a, kind: lax.all_gather(a.astype(kind), axis), x, (jnp.bfloat16, jnp.bfloat16)
    )
    state = jax.tree.map(lambda a, e: jnp.zeros_like(a) + jnp.asarray(e, a.dtype), x, neutral)

    def one(step, state):
        source = count - 1 - step if backward else step
        return join(
            state,
            jax.tree.map(
                lambda a, own: lax.dynamic_index_in_dim(a, source, 0, False).astype(own.dtype),
                gathered,
                x,
            ),
        )

    return lax.fori_loop(0, ahead, one, state)


def block_states(scaled_keys, values_block, running):
    closing = running[:, :, -1:]
    totals = jnp.exp(closing[:, :, 0])
    toward_end = jnp.exp(closing - running).transpose(0, 2, 1)[:, :, :, None]
    from_start = jnp.exp(running).transpose(0, 2, 1)[:, :, :, None]
    forward = jnp.einsum(
        "nshd,nshe->nhde", scaled_keys * toward_end, values_block, precision=HIGHEST
    )
    backward = jnp.einsum(
        "nshd,nshe->nhde", scaled_keys * from_start, values_block, precision=HIGHEST
    )
    return (totals, forward, backward)


def block_outputs(queries, scaled_keys, values_block, running, forward_in, backward_in):
    length = queries.shape[1]
    scores = jnp.einsum("nthd,nshd->nhts", queries, scaled_keys, precision=HIGHEST)
    distance = jnp.abs(running[:, :, :, None] - running[:, :, None, :])
    weights = jnp.exp(-distance) + jnp.eye(length, dtype=jnp.float32)
    within = jnp.einsum("nhts,nshe->nthe", scores * weights, values_block, precision=HIGHEST)
    from_start = jnp.exp(running).transpose(0, 2, 1)[:, :, :, None]
    toward_end = jnp.exp(running[:, :, -1:] - running).transpose(0, 2, 1)[:, :, :, None]
    earlier = jnp.einsum("nthd,nhde->nthe", queries, forward_in, precision=HIGHEST)
    after_part = jnp.einsum("nthd,nhde->nthe", queries, backward_in, precision=HIGHEST)
    return within + from_start * earlier + toward_end * after_part


def head_output(retained, gates_in, head_gain):
    row_count = retained.shape[0]
    centred = retained - jnp.mean(retained, axis=2, keepdims=True)
    scaled = centred * lax.rsqrt(jnp.mean(centred * centred, axis=2, keepdims=True) + EPSILON)
    flattened = scaled.reshape(row_count, -1) * head_gain[None, :]
    return (flattened * jax.nn.silu(gates_in.astype(jnp.float32))).astype(jnp.bfloat16)


def normalize(token_block, input_gain):
    widened = token_block.astype(jnp.float32)
    inverse = lax.rsqrt(jnp.mean(widened * widened, axis=1, keepdims=True) + EPSILON)
    return (widened * inverse * input_gain[None, :]).astype(jnp.bfloat16)


def input_mix(products):
    gated_rows = (products[0] * jax.nn.sigmoid(products[1])).astype(jnp.bfloat16)
    others = [member.astype(jnp.bfloat16) for member in products[2:]]
    return jnp.concatenate([gated_rows] + others, axis=1)


def combine_branches(earlier, latter):
    return (earlier[0] * latter[0], latter[0][:, None, None] * earlier[1] + latter[1])


def fits(tokens, weight, output):
    return (
        lax.axis_size("tp") == 2
        and lax.axis_size("sp") % (SIDE * SIDE) == 0
        and weight.shape == (128, 512)
        and output.shape == (512, 128)
        and tokens.shape[0] % 128 == 0
    )


def general_projections(tokens, input_gain, projections):
    group_rows = lax.all_gather(tokens, "tp", axis=0, tiled=True)
    normed = normalize(group_rows, input_gain)
    portions = (
        lax.all_gather(projections[0], "sp", axis=0, tiled=True),
        lax.all_gather(projections[1], "sp", axis=0, tiled=True),
        lax.all_gather(projections[2], "sp", axis=0, tiled=True),
        lax.all_gather(projections[3], "sp", axis=0, tiled=True),
        lax.all_gather(projections[4], "sp", axis=0, tiled=True),
        lax.all_gather(projections[5], "sp", axis=0, tiled=True),
    )
    return input_mix(
        tuple(
            (jnp.dot(normed, portion, preferred_element_type=jnp.float32) for portion in portions)
        )
    )


def fast_prefix(running, forward, backward):
    count = lax.axis_size("sp")
    me = lax.axis_index("sp")
    heads, width = forward.shape[0], forward.shape[1]
    both_states = jnp.stack([forward, backward]).astype(jnp.bfloat16).reshape(width * 8, -1)
    states = gather_small(count, both_states).reshape(count, 2, heads, width, width)
    logs = jnp.sum(running[:, :, -1], axis=0)
    logs = lax.all_gather(logs, "sp")
    place = jnp.arange(count)
    inner = place[None, :]
    outer = place[:, None]
    left = (inner > outer) & (inner < me)
    right = (inner < outer) & (inner > me)
    left_log = jnp.sum(jnp.where(left[:, :, None], logs[None], 0.0), axis=1)
    right_log = jnp.sum(jnp.where(right[:, :, None], logs[None], 0.0), axis=1)
    left_scale = jnp.where((place < me)[:, None], jnp.exp(left_log), 0.0)
    right_scale = jnp.where((place > me)[:, None], jnp.exp(right_log), 0.0)
    wide = states.astype(jnp.float32)
    enter_left = jnp.sum(left_scale[:, :, None, None] * wide[:, 0], axis=0)
    enter_right = jnp.sum(right_scale[:, :, None, None] * wide[:, 1], axis=0)
    total_left = jnp.exp(jnp.sum(jnp.where((place < me)[:, None], logs, 0.0), axis=0))
    total_right = jnp.exp(jnp.sum(jnp.where((place > me)[:, None], logs, 0.0), axis=0))
    return (total_left, enter_left), (total_right, enter_right)


def body(
    tokens,
    input_gain,
    branch_value,
    branch_gate,
    query_weight,
    key_weight,
    value_weight,
    swish_weight,
    kernel_taps,
    channel_gain,
    decay_logs,
    start_state,
    head_gain,
    output_conv,
    output_heads,
):
    value_width = branch_value.shape[1]
    head_width = query_weight.shape[1]
    fast = fits(tokens, branch_value, output_conv)
    if fast:
        rows = branch_value.shape[0]

        def mixed_columns(a, b):
            return jnp.stack(
                [a.reshape(rows, -1, 128), b.reshape(rows, -1, 128)], axis=2
            ).reshape(rows, -1)

        outputs = jnp.concatenate([output_conv, output_heads], axis=0)
        cut = outputs.shape[1]
        local = jnp.stack(
            [
                mixed_columns(branch_value, branch_gate),
                jnp.concatenate([query_weight, key_weight], axis=1),
                jnp.concatenate([value_weight, swish_weight], axis=1),
                outputs.reshape(-1, cut, cut).transpose(1, 0, 2).reshape(cut, -1),
            ]
        )
        gated_rows, packed, out_weights = project(lax.axis_size("sp"), tokens, input_gain, local)
    else:
        packed = general_projections(
            tokens, input_gain,
            (branch_value, branch_gate, query_weight, key_weight, value_weight, swish_weight),
        )
        gated_rows = packed[:, :value_width]
        packed = packed[:, value_width:]
    row_count = packed.shape[0]
    queries_in = packed[:, :head_width]
    keys_in = packed[:, head_width : 2 * head_width]
    values_in = packed[:, 2 * head_width : 3 * head_width]
    gates_in = packed[:, 3 * head_width :]
    half_width = kernel_taps.shape[0] // 2
    padded = with_halo(gated_rows, (("sp", 0),), half_width).astype(jnp.float32)
    convolved = jnp.zeros((row_count, value_width), jnp.float32)
    for offset in range(kernel_taps.shape[0]):
        convolved = convolved + kernel_taps[offset][None, :] * padded[offset : offset + row_count]
    moments = lax.psum((jnp.sum(convolved, axis=1), jnp.sum(convolved * convolved, axis=1)), "tp")
    average = (moments[0] / DC)[:, None]
    squares = (moments[1] / DC)[:, None]
    normalized = (convolved - average) * lax.rsqrt(squares - average * average + EPSILON)
    branch_out = jax.nn.silu(normalized * channel_gain[None, :]).astype(jnp.bfloat16)
    local_heads = head_width // HD
    blocks = row_count // BLOCK

    def split_heads(matrix):
        return matrix.astype(jnp.float32).reshape(blocks, BLOCK, local_heads, HD)

    query_blocks = split_heads(queries_in)
    key_blocks = split_heads(keys_in) * HD ** (-0.5)
    value_blocks = split_heads(values_in)
    running = jnp.cumsum(decay_logs.reshape(local_heads, blocks, BLOCK).transpose(1, 0, 2), axis=2)
    totals, forward, backward = block_states(key_blocks, value_blocks, running)
    forward_part = []
    forward_scale = []
    carried = jnp.zeros_like(forward[0])
    factor = jnp.ones_like(totals[0])
    for block_index in range(blocks):
        forward_part.append(carried)
        forward_scale.append(factor)
        carried = totals[block_index][:, None, None] * carried + forward[block_index]
        factor = factor * totals[block_index]
    device_forward = carried
    device_total = factor
    backward_part = [None] * blocks
    reverse_direction_scale = [None] * blocks
    carried = jnp.zeros_like(backward[0])
    factor = jnp.ones_like(totals[0])
    for block_index in reversed(range(blocks)):
        backward_part[block_index] = carried
        reverse_direction_scale[block_index] = factor
        carried = totals[block_index][:, None, None] * carried + backward[block_index]
        factor = factor * totals[block_index]
    identity = (jnp.ones_like(device_total), jnp.zeros_like(device_forward))
    if fast:
        before, after = fast_prefix(running, device_forward, carried)
    else:
        before = prefix((device_total, device_forward), "sp", combine_branches, identity, False)
        after = prefix((device_total, carried), "sp", combine_branches, identity, True)
    enter_forward = before[1] + before[0][:, None, None] * start_state[0]
    enter_backward = after[1] + after[0][:, None, None] * start_state[1]
    forward_in = jnp.stack(
        [
            forward_scale[block_index][:, None, None] * enter_forward + forward_part[block_index]
            for block_index in range(blocks)
        ]
    )
    backward_in = jnp.stack(
        [
            reverse_direction_scale[block_index][:, None, None] * enter_backward
            + backward_part[block_index]
            for block_index in range(blocks)
        ]
    )
    retained = block_outputs(
        query_blocks, key_blocks, value_blocks, running, forward_in, backward_in
    )
    heads_out = head_output(retained.reshape(row_count, local_heads, HD), gates_in, head_gain)
    if fast:
        count = lax.axis_size("sp")
        cut = output_conv.shape[1]
        columns = out_weights.reshape(count, cut, -1, cut).transpose(2, 1, 0, 3)
        columns = columns.reshape(-1, count * cut)
        partial_sum = jnp.dot(
            jnp.concatenate([branch_out, heads_out], axis=1),
            columns,
            preferred_element_type=jnp.float32,
        ).astype(jnp.bfloat16)
        halves = partial_sum.reshape(2, row_count // 2, -1)
        core = lax.axis_index("tp")
        mine = lax.dynamic_index_in_dim(halves, core, 0, False)
        other = lax.dynamic_index_in_dim(halves, 1 - core, 0, False)
        received = lax.ppermute(other, "tp", [(0, 1), (1, 0)])
        return (mine.astype(jnp.float32) + received.astype(jnp.float32)).astype(jnp.bfloat16)
    out_columns = (
        lax.all_gather(output_conv, "sp", axis=1, tiled=True),
        lax.all_gather(output_heads, "sp", axis=1, tiled=True),
    )
    combined = jnp.dot(branch_out, out_columns[0], preferred_element_type=jnp.float32)
    return lax.psum_scatter(
        (combined + jnp.dot(heads_out, out_columns[1], preferred_element_type=jnp.float32)).astype(
            jnp.bfloat16
        ),
        "tp",
        scatter_dimension=0,
        tiled=True,
    )


def solution(mesh):
    in_specs = (
        P(("sp", "tp"), None),
        P(),
        P("sp", "tp"),
        P("sp", "tp"),
        P("sp", "tp"),
        P("sp", "tp"),
        P("sp", "tp"),
        P("sp", "tp"),
        P(None, "tp"),
        P("tp"),
        P("tp", "sp"),
        P(None, "tp", None, None),
        P("tp"),
        P("tp", "sp"),
        P("tp", "sp"),
    )
    out_specs = P(("sp", "tp"), None)
    return jax.shard_map(body, mesh=mesh, in_specs=in_specs, out_specs=out_specs, check_vma=False)
```

```python
import functools
import jax
import jax.numpy as jnp
from jax import lax
from jax.experimental import pallas as pl
from jax.experimental.pallas import tpu as pltpu
from jax.sharding import PartitionSpec as P

DC = 1024
HD = 64
BLOCK = 256
SIDE = 2
MESH_ID = pl.DeviceIdType.MESH


class Router:
    def __init__(self, count, rows):
        self.depth = count // (SIDE * SIDE)
        me = lax.axis_index("sp")
        self.x = lax.rem(me, SIDE)
        self.y = lax.rem(me // SIDE, SIDE)
        self.z = me // (SIDE * SIDE)
        tile = 16
        short = rows // (8 * tile) * tile
        long = (rows - 2 * short) // (2 * tile) * tile
        self.routes = (
            ("zxy", 0, rows - 2 * short - long),
            ("zyx", rows - 2 * short - long, long),
            ("xyz", rows - 2 * short, short),
            ("yxz", rows - short, short),
        )
        reach = [(0, None)]
        for d in range(1, self.depth):
            reach += [(-d, self.z - d >= 0), (d, self.z + d < self.depth)]
        self.events = []
        for dz, valid in reach:
            for dy in range(SIDE):
                for dx in range(SIDE):
                    if dz == dy == dx == 0:
                        continue
                    for r, (order, _, _) in enumerate(self.routes):
                        self.events.append((abs(dz) + dy + dx, r, dz, dy, dx, valid))
        self.events.sort(key=lambda e: (e[0], e[1], e[2], e[3], e[4]))

    def index(self, z, y, x):
        return (z * SIDE + y) * SIDE + x

    def source(self, dz, dy, dx):
        y = self.y if dy == 0 else 1 - self.y
        x = self.x if dx == 0 else 1 - self.x
        return self.index(self.z + dz, y, x)

    def neighbours(self):
        z, y, x = self.z, self.y, self.x
        return {
            "x": (self.index(z, y, 1 - x), None),
            "y": (self.index(z, 1 - y, x), None),
            "+": (self.index(z + 1, y, x), z + 1 < self.depth),
            "-": (self.index(z - 1, y, x), z - 1 >= 0),
        }

    def targets(self, r, dz, dy, dx):
        order = self.routes[r][0]
        off = {"z": dz, "y": dy, "x": dx}
        last = max([i for i, d in enumerate(order) if off[d] != 0], default=-1)
        out = []
        if last >= 0 and order[last] == "z":
            out.append("+" if dz < 0 else "-")
        for d in order[last + 1 :]:
            out += ["+", "-"] if d == "z" else [d]
        return out


def when(cond, fn):
    if cond is None:
        fn()
    else:
        pl.when(cond)(fn)


def both(a, b):
    if a is None:
        return b
    if b is None:
        return a
    return jnp.logical_and(a, b)


DIRECTIONS = "xy+-"


def enter(router, partner):
    barrier = pltpu.get_barrier_semaphore()
    near = router.neighbours()
    for idx, valid in near.values():

        def greet(idx=idx):
            pl.semaphore_signal(barrier, inc=1, device_id={"sp": idx}, device_id_type=MESH_ID)

        when(valid, greet)
    extra = 0
    if partner is not None:
        pl.semaphore_signal(barrier, inc=1, device_id={"tp": partner}, device_id_type=MESH_ID)
        extra = 1
    ends = sum(jnp.where(near[d][1], 1, 0) for d in "+-")
    pl.semaphore_wait(barrier, 2 + extra + ends)


class Flow:
    def __init__(self, router, local, gathered, rows, send_sem, recv_sem):
        self.router, self.local, self.gathered, self.rows = router, local, gathered, rows
        self.send_sem, self.recv_sem = send_sem, recv_sem

    def copy(self, g, r, dz, dy, dx, d):
        router = self.router
        _, first, count = router.routes[r]
        s = router.source(dz, dy, dx)
        place = self.gathered.at[g, s, pl.ds(first, count), :]
        src = self.local.at[g, pl.ds(first, count), :] if dz == dy == dx == 0 else place
        idx, valid = router.neighbours()[d]
        k = DIRECTIONS.index(d)
        return (
            pltpu.make_async_remote_copy(
                src_ref=src,
                dst_ref=place,
                send_sem=self.send_sem.at[g, r, k, s],
                recv_sem=self.recv_sem.at[g, r, s],
                device_id={"sp": idx},
                device_id_type=MESH_ID,
            ),
            valid,
        )

    def send(self, g, r, dz, dy, dx, wait=False):
        for d in self.router.targets(r, dz, dy, dx):
            copy, valid = self.copy(g, r, dz, dy, dx, d)
            when(valid, copy.wait_send if wait else copy.start)

    def own(self, g, wait=False):
        for r in range(len(self.router.routes)):
            self.send(g, r, 0, 0, 0, wait)

    def event(self, g, e):
        _, r, dz, dy, dx, cond = e

        def arrived():
            self.copy(g, r, dz, dy, dx, "x")[0].wait_recv()
            self.send(g, r, dz, dy, dx)

        when(cond, arrived)

    def finish(self, g):
        self.own(g, True)
        for e in self.router.events:
            _, r, dz, dy, dx, cond = e
            if self.router.targets(r, dz, dy, dx):
                when(cond, functools.partial(self.send, g, r, dz, dy, dx, True))


def project_kernel(
    count, tokens, gain, local, gated_out, packed_out, last_out,
    gathered, raw, normed, send_sem, recv_sem, local_sem, swap_sem,
):
    groups, rows, width = local.shape
    router = Router(count, rows)
    core = lax.axis_index("tp")
    partner = 1 - core
    own_rows = tokens.shape[0]
    flow = Flow(router, local, gathered, rows, send_sem, recv_sem)
    mine = pl.ds(pl.multiple_of(core * own_rows, own_rows), own_rows)
    me = lax.axis_index("sp")
    enter(router, partner)
    flow.own(0)
    swap = pltpu.make_async_remote_copy(
        src_ref=tokens, dst_ref=raw.at[mine, :], send_sem=swap_sem.at[0], recv_sem=swap_sem.at[1],
        device_id={"tp": partner}, device_id_type=MESH_ID,
    )
    swap.start()
    keep = pltpu.make_async_copy(tokens, raw.at[mine, :], local_sem.at[groups])
    keep.start()
    for g in range(groups):
        pltpu.make_async_copy(local.at[g], gathered.at[g, me], local_sem.at[g]).start()
    for g in range(groups):
        pltpu.make_async_copy(local.at[g], gathered.at[g, me], local_sem.at[g]).wait()
    keep.wait()
    swap.wait()
    n_events = len(router.events)
    half = normed.shape[0] // 2
    tiles = width // 256
    units = 2 * tiles
    norm_rows = normed.shape[0] // units

    def unit(it, u):
        @pl.when(it == 0)
        def _():
            window = pl.ds(u * norm_rows, norm_rows)
            widened = raw[window, :].astype(jnp.float32)
            inverse = lax.rsqrt(jnp.mean(widened * widened, axis=1, keepdims=True) + EPSILON)
            normed[window, :] = (widened * inverse * gain[...]).astype(jnp.bfloat16)

        @pl.when(it > 0)
        def _():
            m, n = u % 2, u // 2
            window = pl.ds(m * half, half)
            weight = gathered[it - 1, :, :, n * 256 : (n + 1) * 256].reshape(count * rows, 256)
            product = jnp.dot(normed[window, :], weight, preferred_element_type=jnp.float32)

            @pl.when(it == 1)
            def _():
                gated_out[window, n * 128 : (n + 1) * 128] = (
                    product[:, :128] * jax.nn.sigmoid(product[:, 128:])
                ).astype(jnp.bfloat16)

            @pl.when(it > 1)
            def _():
                column = pl.multiple_of((it - 2) * width + n * 256, 256)
                packed_out[window, pl.ds(column, 256)] = product.astype(jnp.bfloat16)

    def step(it, _):
        @pl.when(it < groups - 1)
        def _():
            flow.own(it + 1)

        done = 0
        for i, e in enumerate(router.events):
            flow.event(it, e)
            while done < units and (i + 1) * units >= (done + 1) * n_events:
                unit(it, done)
                done += 1
        return 0

    lax.fori_loop(0, groups, step, 0)
    last = gathered.at[groups - 1]

    def place(s, _):
        for j in range(width // rows):
            pltpu.make_async_copy(
                last.at[s, :, pl.ds(j * rows, rows)],
                last_out.at[pl.ds(j * rows, rows), pl.ds(pl.multiple_of(s * rows, rows), rows)],
                local_sem.at[0],
            ).start()
        return 0

    lax.fori_loop(0, count, place, 0)

    def drain(g, _):
        flow.finish(g)
        return 0

    lax.fori_loop(0, groups, drain, 0)
    pltpu.make_async_copy(last, last, local_sem.at[0]).wait()


def project(count, tokens, gain, local):
    groups, rows, width = local.shape
    total = tokens.shape[0] * 2
    model = tokens.shape[1]
    vmem = pl.BlockSpec(memory_space=pltpu.VMEM)
    return pl.pallas_call(
        functools.partial(project_kernel, count),
        out_shape=(
            jax.ShapeDtypeStruct((total, width // 2), jnp.bfloat16),
            jax.ShapeDtypeStruct((total, (groups - 2) * width), jnp.bfloat16),
            jax.ShapeDtypeStruct((width, count * rows), jnp.bfloat16),
        ),
        in_specs=[vmem] * 3,
        out_specs=(vmem, vmem, pl.BlockSpec(memory_space=pl.ANY)),
        scratch_shapes=[
            pltpu.VMEM((groups, count, rows, width), jnp.bfloat16),
            pltpu.VMEM((total, model), jnp.bfloat16),
            pltpu.VMEM((total, model), jnp.bfloat16),
            pltpu.SemaphoreType.DMA((groups, 4, 4, count)),
            pltpu.SemaphoreType.DMA((groups, 4, count)),
            pltpu.SemaphoreType.DMA((groups + 1,)),
            pltpu.SemaphoreType.DMA((2,)),
        ],
        compiler_params=pltpu.CompilerParams(
            collective_id=0, has_side_effects=True, vmem_limit_bytes=60 * 1024 * 1024
        ),
        name="project",
    )(tokens, gain.reshape(1, -1), local)


def gather_kernel(count, local, gathered, send_sem, recv_sem, local_sem):
    _, rows, _ = local.shape
    router = Router(count, rows)
    flow = Flow(router, local, gathered, rows, send_sem, recv_sem)
    enter(router, None)
    flow.own(0)
    keep = pltpu.make_async_copy(local.at[0], gathered.at[0, lax.axis_index("sp")], local_sem.at[0])
    keep.start()
    for e in router.events:
        flow.event(0, e)
    keep.wait()
    flow.finish(0)


def gather_small(count, local):
    rows, width = local.shape
    vmem = pl.BlockSpec(memory_space=pltpu.VMEM)
    return pl.pallas_call(
        functools.partial(gather_kernel, count),
        out_shape=jax.ShapeDtypeStruct((1, count, rows, width), local.dtype),
        in_specs=[vmem],
        out_specs=vmem,
        scratch_shapes=[
            pltpu.SemaphoreType.DMA((1, 4, 4, count)),
            pltpu.SemaphoreType.DMA((1, 4, count)),
            pltpu.SemaphoreType.DMA((1,)),
        ],
        compiler_params=pltpu.CompilerParams(collective_id=1, has_side_effects=True),
        name="gather_states",
    )(local[None])[0]


EPSILON = 1e-06
HIGHEST = lax.Precision.HIGHEST


def with_halo(x, sides, width):
    for axis, dim in sides:
        count, length = (lax.axis_size(axis), x.shape[dim])
        up = [(i, (i + 1) % count) for i in range(count - 1)]
        down = [(j, i) for i, j in up]
        last = lax.slice_in_dim(x, length - width, length, axis=dim)
        first = lax.slice_in_dim(x, 0, width, axis=dim)
        before = lax.ppermute(last, axis, up)
        after = lax.ppermute(first, axis, down)
        x = jnp.concatenate([before, x, after], axis=dim)
    return x


def prefix(x, axis, join, neutral, backward):
    count = lax.axis_size(axis)
    place = lax.axis_index(axis)
    ahead = count - 1 - place if backward else place
    gathered = jax.tree.map(
        lambda a, kind: lax.all_gather(a.astype(kind), axis), x, (jnp.bfloat16, jnp.bfloat16)
    )
    state = jax.tree.map(lambda a, e: jnp.zeros_like(a) + jnp.asarray(e, a.dtype), x, neutral)

    def one(step, state):
        source = count - 1 - step if backward else step
        return join(
            state,
            jax.tree.map(
                lambda a, own: lax.dynamic_index_in_dim(a, source, 0, False).astype(own.dtype),
                gathered,
                x,
            ),
        )

    return lax.fori_loop(0, ahead, one, state)


def block_states(scaled_keys, values_block, running):
    closing = running[:, :, -1:]
    totals = jnp.exp(closing[:, :, 0])
    toward_end = jnp.exp(closing - running).transpose(0, 2, 1)[:, :, :, None]
    from_start = jnp.exp(running).transpose(0, 2, 1)[:, :, :, None]
    forward = jnp.einsum(
        "nshd,nshe->nhde", scaled_keys * toward_end, values_block, precision=HIGHEST
    )
    backward = jnp.einsum(
        "nshd,nshe->nhde", scaled_keys * from_start, values_block, precision=HIGHEST
    )
    return (totals, forward, backward)


def block_outputs(queries, scaled_keys, values_block, running, forward_in, backward_in):
    length = queries.shape[1]
    scores = jnp.einsum("nthd,nshd->nhts", queries, scaled_keys, precision=HIGHEST)
    distance = jnp.abs(running[:, :, :, None] - running[:, :, None, :])
    weights = jnp.exp(-distance) + jnp.eye(length, dtype=jnp.float32)
    within = jnp.einsum("nhts,nshe->nthe", scores * weights, values_block, precision=HIGHEST)
    from_start = jnp.exp(running).transpose(0, 2, 1)[:, :, :, None]
    toward_end = jnp.exp(running[:, :, -1:] - running).transpose(0, 2, 1)[:, :, :, None]
    earlier = jnp.einsum("nthd,nhde->nthe", queries, forward_in, precision=HIGHEST)
    after_part = jnp.einsum("nthd,nhde->nthe", queries, backward_in, precision=HIGHEST)
    return within + from_start * earlier + toward_end * after_part


def head_output(retained, gates_in, head_gain):
    row_count = retained.shape[0]
    centred = retained - jnp.mean(retained, axis=2, keepdims=True)
    scaled = centred * lax.rsqrt(jnp.mean(centred * centred, axis=2, keepdims=True) + EPSILON)
    flattened = scaled.reshape(row_count, -1) * head_gain[None, :]
    return (flattened * jax.nn.silu(gates_in.astype(jnp.float32))).astype(jnp.bfloat16)


def normalize(token_block, input_gain):
    widened = token_block.astype(jnp.float32)
    inverse = lax.rsqrt(jnp.mean(widened * widened, axis=1, keepdims=True) + EPSILON)
    return (widened * inverse * input_gain[None, :]).astype(jnp.bfloat16)


def input_mix(products):
    gated_rows = (products[0] * jax.nn.sigmoid(products[1])).astype(jnp.bfloat16)
    others = [member.astype(jnp.bfloat16) for member in products[2:]]
    return jnp.concatenate([gated_rows] + others, axis=1)


def combine_branches(earlier, latter):
    return (earlier[0] * latter[0], latter[0][:, None, None] * earlier[1] + latter[1])


def states_kernel(packed, end_scale, start_scale, forward, backward):
    rows, wide = packed.shape
    width = wide // 4
    pair = 2 * HD
    first = lax.broadcasted_iota(jnp.int32, (rows, pair), 1) < HD
    for h in range(0, width // HD, 2):
        at = h * HD
        keys = packed[:, width + at : width + at + pair].astype(jnp.float32) * HD ** (-0.5)
        values = packed[:, 2 * width + at : 2 * width + at + pair]
        for scale, out in ((end_scale, forward), (start_scale, backward)):
            factor = jnp.where(first, scale[:, h : h + 1], scale[:, h + 1 : h + 2])
            state = lax.dot_general(
                (keys * factor).astype(jnp.bfloat16), values, (((0,), (0,)), ((), ())),
                preferred_element_type=jnp.float32,
            )
            out[0, h] = state[:HD, :HD]
            out[0, h + 1] = state[HD:, HD:]


def fast_states(packed, running):
    blocks, heads, length = running.shape
    closing = running[:, :, -1:]
    end_scale = jnp.exp(closing - running).transpose(0, 2, 1).reshape(-1, heads)
    start_scale = jnp.exp(running).transpose(0, 2, 1).reshape(-1, heads)
    rows = pl.BlockSpec((length, packed.shape[1]), lambda n: (n, 0))
    scale = pl.BlockSpec((length, heads), lambda n: (n, 0))
    state = pl.BlockSpec((1, heads, HD, HD), lambda n: (n, 0, 0, 0))
    shape = jax.ShapeDtypeStruct((blocks, heads, HD, HD), jnp.float32)
    forward, backward = pl.pallas_call(
        states_kernel, grid=(blocks,), in_specs=[rows, scale, scale],
        out_specs=(state, state), out_shape=(shape, shape), name="block_states",
    )(packed, end_scale, start_scale)
    return jnp.exp(closing[:, :, 0]), forward, backward


def retain_kernel(packed, column, row, forward_in, backward_in, gain, out):
    rows, wide = packed.shape
    width = wide // 4
    pair = 2 * HD
    t = lax.broadcasted_iota(jnp.int32, (rows, rows), 0)
    s = lax.broadcasted_iota(jnp.int32, (rows, rows), 1)
    same = jnp.where(t == s, 1.0, 0.0)
    for h in range(0, width // HD, 2):
        at = h * HD
        q, k, v, g = (packed[:, i * width + at : i * width + at + pair] for i in range(4))
        done = []
        for i in range(2):
            lanes = slice(i * HD, (i + 1) * HD)
            head = h + i
            scores = lax.dot_general(
                q[:, lanes], k[:, lanes], (((1,), (1,)), ((), ())),
                preferred_element_type=jnp.float32,
            ) * HD ** (-0.5)
            down = column[:, head : head + 1]
            along = row[0, head : head + 1, :]
            weights = jnp.exp(-jnp.abs(down - along)) + same
            within = jnp.dot(
                (scores * weights).astype(jnp.bfloat16), v[:, lanes],
                preferred_element_type=jnp.float32,
            )
            entering = [
                jnp.dot(q[:, lanes], state[0, head].astype(jnp.bfloat16),
                        preferred_element_type=jnp.float32)
                for state in (forward_in, backward_in)
            ]
            closing = column[rows - 1 : rows, head : head + 1]
            kept = within + jnp.exp(down) * entering[0] + jnp.exp(closing - down) * entering[1]
            centred = kept - jnp.mean(kept, axis=1, keepdims=True)
            done.append(
                centred * lax.rsqrt(jnp.mean(centred * centred, axis=1, keepdims=True) + EPSILON)
            )
        both_heads = jnp.concatenate(done, axis=1) * gain[:, at : at + pair]
        out[:, at : at + pair] = (both_heads * jax.nn.silu(g.astype(jnp.float32))).astype(
            jnp.bfloat16
        )


def fast_retention(packed, running, forward_in, backward_in, head_gain):
    blocks, heads, length = running.shape
    column = running.transpose(0, 2, 1).reshape(-1, heads)
    width = heads * HD
    state = pl.BlockSpec((1, heads, HD, HD), lambda n: (n, 0, 0, 0))
    return pl.pallas_call(
        retain_kernel, grid=(blocks,),
        in_specs=[
            pl.BlockSpec((length, packed.shape[1]), lambda n: (n, 0)),
            pl.BlockSpec((length, heads), lambda n: (n, 0)),
            pl.BlockSpec((1, heads, length), lambda n: (n, 0, 0)),
            state, state,
            pl.BlockSpec((1, width), lambda n: (0, 0)),
        ],
        out_specs=pl.BlockSpec((length, width), lambda n: (n, 0)),
        out_shape=jax.ShapeDtypeStruct((packed.shape[0], width), jnp.bfloat16),
        name="retain",
    )(packed, column, running, forward_in, backward_in, head_gain.reshape(1, -1))


def fits(tokens, weight, output):
    return (
        lax.axis_size("tp") == 2
        and lax.axis_size("sp") % (SIDE * SIDE) == 0
        and weight.shape == (128, 512)
        and output.shape == (512, 128)
        and tokens.shape[0] % 128 == 0
    )


def general_projections(tokens, input_gain, projections):
    group_rows = lax.all_gather(tokens, "tp", axis=0, tiled=True)
    normed = normalize(group_rows, input_gain)
    portions = (
        lax.all_gather(projections[0], "sp", axis=0, tiled=True),
        lax.all_gather(projections[1], "sp", axis=0, tiled=True),
        lax.all_gather(projections[2], "sp", axis=0, tiled=True),
        lax.all_gather(projections[3], "sp", axis=0, tiled=True),
        lax.all_gather(projections[4], "sp", axis=0, tiled=True),
        lax.all_gather(projections[5], "sp", axis=0, tiled=True),
    )
    return input_mix(
        tuple(
            (jnp.dot(normed, portion, preferred_element_type=jnp.float32) for portion in portions)
        )
    )


def fast_prefix(running, forward, backward):
    count = lax.axis_size("sp")
    me = lax.axis_index("sp")
    heads, width = forward.shape[0], forward.shape[1]
    logs = jnp.sum(running[:, :, -1], axis=0)
    coarse = lax.reduce_precision(logs, 8, 7)
    pair = jnp.concatenate([coarse, logs - coarse]).astype(jnp.bfloat16)
    extra = jnp.zeros((16, 128), jnp.bfloat16).at[0, : 2 * heads].set(pair)
    both_states = jnp.stack([forward, backward]).astype(jnp.bfloat16).reshape(-1, 128)
    cut = both_states.shape[0]
    arrived = gather_small(count, jnp.concatenate([both_states, extra], axis=0))
    states = arrived[:, :cut].reshape(count, 2, heads, width, width)
    pair = arrived[:, cut, : 2 * heads].astype(jnp.float32)
    logs = pair[:, :heads] + pair[:, heads:]
    place = jnp.arange(count)
    inner = place[None, :]
    outer = place[:, None]
    left = (inner > outer) & (inner < me)
    right = (inner < outer) & (inner > me)
    left_log = jnp.sum(jnp.where(left[:, :, None], logs[None], 0.0), axis=1)
    right_log = jnp.sum(jnp.where(right[:, :, None], logs[None], 0.0), axis=1)
    left_scale = jnp.where((place < me)[:, None], jnp.exp(left_log), 0.0)
    right_scale = jnp.where((place > me)[:, None], jnp.exp(right_log), 0.0)
    wide = states.astype(jnp.float32)
    enter_left = jnp.sum(left_scale[:, :, None, None] * wide[:, 0], axis=0)
    enter_right = jnp.sum(right_scale[:, :, None, None] * wide[:, 1], axis=0)
    total_left = jnp.exp(jnp.sum(jnp.where((place < me)[:, None], logs, 0.0), axis=0))
    total_right = jnp.exp(jnp.sum(jnp.where((place > me)[:, None], logs, 0.0), axis=0))
    return (total_left, enter_left), (total_right, enter_right)


def body(
    tokens,
    input_gain,
    branch_value,
    branch_gate,
    query_weight,
    key_weight,
    value_weight,
    swish_weight,
    kernel_taps,
    channel_gain,
    decay_logs,
    start_state,
    head_gain,
    output_conv,
    output_heads,
):
    value_width = branch_value.shape[1]
    head_width = query_weight.shape[1]
    fast = fits(tokens, branch_value, output_conv)
    if fast:
        rows = branch_value.shape[0]

        def mixed_columns(a, b):
            return jnp.stack(
                [a.reshape(rows, -1, 128), b.reshape(rows, -1, 128)], axis=2
            ).reshape(rows, -1)

        outputs = jnp.concatenate([output_conv, output_heads], axis=0)
        cut = outputs.shape[1]
        local = jnp.stack(
            [
                mixed_columns(branch_value, branch_gate),
                jnp.concatenate([query_weight, key_weight], axis=1),
                jnp.concatenate([value_weight, swish_weight], axis=1),
                outputs.reshape(-1, cut, cut).transpose(1, 0, 2).reshape(cut, -1),
            ]
        )
        gated_rows, packed, out_weights = project(lax.axis_size("sp"), tokens, input_gain, local)
    else:
        packed = general_projections(
            tokens, input_gain,
            (branch_value, branch_gate, query_weight, key_weight, value_weight, swish_weight),
        )
        gated_rows = packed[:, :value_width]
        packed = packed[:, value_width:]
    row_count = packed.shape[0]
    queries_in = packed[:, :head_width]
    keys_in = packed[:, head_width : 2 * head_width]
    values_in = packed[:, 2 * head_width : 3 * head_width]
    gates_in = packed[:, 3 * head_width :]
    half_width = kernel_taps.shape[0] // 2
    padded = with_halo(gated_rows, (("sp", 0),), half_width).astype(jnp.float32)
    convolved = jnp.zeros((row_count, value_width), jnp.float32)
    for offset in range(kernel_taps.shape[0]):
        convolved = convolved + kernel_taps[offset][None, :] * padded[offset : offset + row_count]
    moments = lax.psum((jnp.sum(convolved, axis=1), jnp.sum(convolved * convolved, axis=1)), "tp")
    average = (moments[0] / DC)[:, None]
    squares = (moments[1] / DC)[:, None]
    normalized = (convolved - average) * lax.rsqrt(squares - average * average + EPSILON)
    branch_out = jax.nn.silu(normalized * channel_gain[None, :]).astype(jnp.bfloat16)
    local_heads = head_width // HD
    blocks = row_count // BLOCK

    def split_heads(matrix):
        return matrix.astype(jnp.float32).reshape(blocks, BLOCK, local_heads, HD)

    query_blocks = split_heads(queries_in)
    key_blocks = split_heads(keys_in) * HD ** (-0.5)
    value_blocks = split_heads(values_in)
    running = jnp.cumsum(decay_logs.reshape(local_heads, blocks, BLOCK).transpose(1, 0, 2), axis=2)
    if fast:
        totals, forward, backward = fast_states(packed, running)
    else:
        totals, forward, backward = block_states(key_blocks, value_blocks, running)
    forward_part = []
    forward_scale = []
    carried = jnp.zeros_like(forward[0])
    factor = jnp.ones_like(totals[0])
    for block_index in range(blocks):
        forward_part.append(carried)
        forward_scale.append(factor)
        carried = totals[block_index][:, None, None] * carried + forward[block_index]
        factor = factor * totals[block_index]
    device_forward = carried
    device_total = factor
    backward_part = [None] * blocks
    reverse_direction_scale = [None] * blocks
    carried = jnp.zeros_like(backward[0])
    factor = jnp.ones_like(totals[0])
    for block_index in reversed(range(blocks)):
        backward_part[block_index] = carried
        reverse_direction_scale[block_index] = factor
        carried = totals[block_index][:, None, None] * carried + backward[block_index]
        factor = factor * totals[block_index]
    identity = (jnp.ones_like(device_total), jnp.zeros_like(device_forward))
    if fast:
        before, after = fast_prefix(running, device_forward, carried)
    else:
        before = prefix((device_total, device_forward), "sp", combine_branches, identity, False)
        after = prefix((device_total, carried), "sp", combine_branches, identity, True)
    enter_forward = before[1] + before[0][:, None, None] * start_state[0]
    enter_backward = after[1] + after[0][:, None, None] * start_state[1]
    forward_in = jnp.stack(
        [
            forward_scale[block_index][:, None, None] * enter_forward + forward_part[block_index]
            for block_index in range(blocks)
        ]
    )
    backward_in = jnp.stack(
        [
            reverse_direction_scale[block_index][:, None, None] * enter_backward
            + backward_part[block_index]
            for block_index in range(blocks)
        ]
    )
    if fast:
        heads_out = fast_retention(packed, running, forward_in, backward_in, head_gain)
    else:
        retained = block_outputs(
            query_blocks, key_blocks, value_blocks, running, forward_in, backward_in
        )
        heads_out = head_output(retained.reshape(row_count, local_heads, HD), gates_in, head_gain)
    if fast:
        partial_sum = jnp.dot(
            jnp.concatenate([branch_out, heads_out], axis=1),
            out_weights,
            preferred_element_type=jnp.float32,
        ).astype(jnp.bfloat16)
        halves = partial_sum.reshape(2, row_count // 2, -1)
        core = lax.axis_index("tp")
        mine = lax.dynamic_index_in_dim(halves, core, 0, False)
        other = lax.dynamic_index_in_dim(halves, 1 - core, 0, False)
        received = lax.ppermute(other, "tp", [(0, 1), (1, 0)])
        return (mine.astype(jnp.float32) + received.astype(jnp.float32)).astype(jnp.bfloat16)
    out_columns = (
        lax.all_gather(output_conv, "sp", axis=1, tiled=True),
        lax.all_gather(output_heads, "sp", axis=1, tiled=True),
    )
    combined = jnp.dot(branch_out, out_columns[0], preferred_element_type=jnp.float32)
    return lax.psum_scatter(
        (combined + jnp.dot(heads_out, out_columns[1], preferred_element_type=jnp.float32)).astype(
            jnp.bfloat16
        ),
        "tp",
        scatter_dimension=0,
        tiled=True,
    )


def solution(mesh):
    in_specs = (
        P(("sp", "tp"), None),
        P(),
        P("sp", "tp"),
        P("sp", "tp"),
        P("sp", "tp"),
        P("sp", "tp"),
        P("sp", "tp"),
        P("sp", "tp"),
        P(None, "tp"),
        P("tp"),
        P("tp", "sp"),
        P(None, "tp", None, None),
        P("tp"),
        P("tp", "sp"),
        P("tp", "sp"),
    )
    out_specs = P(("sp", "tp"), None)
    return jax.shard_map(body, mesh=mesh, in_specs=in_specs, out_specs=out_specs, check_vma=False)
```

```python
import functools
import jax
import jax.numpy as jnp
from jax import lax
from jax.experimental import pallas as pl
from jax.experimental.pallas import tpu as pltpu
from jax.sharding import PartitionSpec as P

DC = 1024
HD = 64
BLOCK = 256
SIDE = 2
MESH_ID = pl.DeviceIdType.MESH


class Router:
    def __init__(self, count, rows):
        self.depth = count // (SIDE * SIDE)
        me = lax.axis_index("sp")
        self.x = lax.rem(me, SIDE)
        self.y = lax.rem(me // SIDE, SIDE)
        self.z = me // (SIDE * SIDE)
        tile = 16
        short = rows // (8 * tile) * tile
        long = (rows - 2 * short) // (2 * tile) * tile
        self.routes = (
            ("zxy", 0, rows - 2 * short - long),
            ("zyx", rows - 2 * short - long, long),
            ("xyz", rows - 2 * short, short),
            ("yxz", rows - short, short),
        )
        reach = [(0, None)]
        for d in range(1, self.depth):
            reach += [(-d, self.z - d >= 0), (d, self.z + d < self.depth)]
        self.events = []
        for dz, valid in reach:
            for dy in range(SIDE):
                for dx in range(SIDE):
                    if dz == dy == dx == 0:
                        continue
                    for r, (order, _, _) in enumerate(self.routes):
                        self.events.append((abs(dz) + dy + dx, r, dz, dy, dx, valid))
        self.events.sort(key=lambda e: (e[0], e[1], e[2], e[3], e[4]))

    def index(self, z, y, x):
        return (z * SIDE + y) * SIDE + x

    def source(self, dz, dy, dx):
        y = self.y if dy == 0 else 1 - self.y
        x = self.x if dx == 0 else 1 - self.x
        return self.index(self.z + dz, y, x)

    def neighbours(self):
        z, y, x = self.z, self.y, self.x
        return {
            "x": (self.index(z, y, 1 - x), None),
            "y": (self.index(z, 1 - y, x), None),
            "+": (self.index(z + 1, y, x), z + 1 < self.depth),
            "-": (self.index(z - 1, y, x), z - 1 >= 0),
        }

    def targets(self, r, dz, dy, dx):
        order = self.routes[r][0]
        off = {"z": dz, "y": dy, "x": dx}
        last = max([i for i, d in enumerate(order) if off[d] != 0], default=-1)
        out = []
        if last >= 0 and order[last] == "z":
            out.append("+" if dz < 0 else "-")
        for d in order[last + 1 :]:
            out += ["+", "-"] if d == "z" else [d]
        return out


def when(cond, fn):
    if cond is None:
        fn()
    else:
        pl.when(cond)(fn)


def both(a, b):
    if a is None:
        return b
    if b is None:
        return a
    return jnp.logical_and(a, b)


DIRECTIONS = "xy+-"


def enter(router, partner):
    barrier = pltpu.get_barrier_semaphore()
    near = router.neighbours()
    for idx, valid in near.values():

        def greet(idx=idx):
            pl.semaphore_signal(barrier, inc=1, device_id={"sp": idx}, device_id_type=MESH_ID)

        when(valid, greet)
    extra = 0
    if partner is not None:
        pl.semaphore_signal(barrier, inc=1, device_id={"tp": partner}, device_id_type=MESH_ID)
        extra = 1
    ends = sum(jnp.where(near[d][1], 1, 0) for d in "+-")
    pl.semaphore_wait(barrier, 2 + extra + ends)


class Flow:
    def __init__(self, router, local, gathered, rows, send_sem, recv_sem):
        self.router, self.local, self.gathered, self.rows = router, local, gathered, rows
        self.send_sem, self.recv_sem = send_sem, recv_sem

    def copy(self, g, r, dz, dy, dx, d):
        router = self.router
        _, first, count = router.routes[r]
        s = router.source(dz, dy, dx)
        place = self.gathered.at[g, s, pl.ds(first, count), :]
        src = self.local.at[g, pl.ds(first, count), :] if dz == dy == dx == 0 else place
        idx, valid = router.neighbours()[d]
        k = DIRECTIONS.index(d)
        return (
            pltpu.make_async_remote_copy(
                src_ref=src,
                dst_ref=place,
                send_sem=self.send_sem.at[g, r, k, s],
                recv_sem=self.recv_sem.at[g, r, s],
                device_id={"sp": idx},
                device_id_type=MESH_ID,
            ),
            valid,
        )

    def send(self, g, r, dz, dy, dx, wait=False):
        for d in self.router.targets(r, dz, dy, dx):
            copy, valid = self.copy(g, r, dz, dy, dx, d)
            when(valid, copy.wait_send if wait else copy.start)

    def own(self, g, wait=False):
        for r in range(len(self.router.routes)):
            self.send(g, r, 0, 0, 0, wait)

    def event(self, g, e):
        _, r, dz, dy, dx, cond = e

        def arrived():
            self.copy(g, r, dz, dy, dx, "x")[0].wait_recv()
            self.send(g, r, dz, dy, dx)

        when(cond, arrived)

    def finish(self, g):
        self.own(g, True)
        for e in self.router.events:
            _, r, dz, dy, dx, cond = e
            if self.router.targets(r, dz, dy, dx):
                when(cond, functools.partial(self.send, g, r, dz, dy, dx, True))


def project_kernel(
    count, tokens, gain, local, gated_out, packed_out, last_out,
    gathered, raw, normed, send_sem, recv_sem, local_sem, swap_sem,
):
    groups, rows, width = local.shape
    router = Router(count, rows)
    core = lax.axis_index("tp")
    partner = 1 - core
    own_rows = tokens.shape[0]
    flow = Flow(router, local, gathered, rows, send_sem, recv_sem)
    mine = pl.ds(pl.multiple_of(core * own_rows, own_rows), own_rows)
    me = lax.axis_index("sp")
    enter(router, partner)
    flow.own(0)
    swap = pltpu.make_async_remote_copy(
        src_ref=tokens, dst_ref=raw.at[mine, :], send_sem=swap_sem.at[0], recv_sem=swap_sem.at[1],
        device_id={"tp": partner}, device_id_type=MESH_ID,
    )
    swap.start()
    keep = pltpu.make_async_copy(tokens, raw.at[mine, :], local_sem.at[groups])
    keep.start()
    for g in range(groups):
        pltpu.make_async_copy(local.at[g], gathered.at[g, me], local_sem.at[g]).start()
    for g in range(groups):
        pltpu.make_async_copy(local.at[g], gathered.at[g, me], local_sem.at[g]).wait()
    keep.wait()
    swap.wait()
    n_events = len(router.events)
    half = normed.shape[0] // 2
    tiles = width // 256
    units = 2 * tiles
    norm_rows = normed.shape[0] // units

    def unit(it, u):
        @pl.when(it == 0)
        def _():
            window = pl.ds(u * norm_rows, norm_rows)
            widened = raw[window, :].astype(jnp.float32)
            inverse = lax.rsqrt(jnp.mean(widened * widened, axis=1, keepdims=True) + EPSILON)
            normed[window, :] = (widened * inverse * gain[...]).astype(jnp.bfloat16)

        @pl.when(it > 0)
        def _():
            m, n = u % 2, u // 2
            window = pl.ds(m * half, half)
            weight = gathered[it - 1, :, :, n * 256 : (n + 1) * 256].reshape(count * rows, 256)
            product = jnp.dot(normed[window, :], weight, preferred_element_type=jnp.float32)

            @pl.when(it == 1)
            def _():
                gated_out[window, n * 128 : (n + 1) * 128] = (
                    product[:, :128] * jax.nn.sigmoid(product[:, 128:])
                ).astype(jnp.bfloat16)

            @pl.when(it > 1)
            def _():
                column = pl.multiple_of((it - 2) * width + n * 256, 256)
                packed_out[window, pl.ds(column, 256)] = product.astype(jnp.bfloat16)

    def step(it, _):
        @pl.when(it < groups - 1)
        def _():
            flow.own(it + 1)

        done = 0
        for i, e in enumerate(router.events):
            flow.event(it, e)
            while done < units and (i + 1) * units >= (done + 1) * n_events:
                unit(it, done)
                done += 1
        return 0

    lax.fori_loop(0, groups, step, 0)
    last = gathered.at[groups - 1]

    def place(s, _):
        for j in range(width // rows):
            pltpu.make_async_copy(
                last.at[s, :, pl.ds(j * rows, rows)],
                last_out.at[pl.ds(j * rows, rows), pl.ds(pl.multiple_of(s * rows, rows), rows)],
                local_sem.at[0],
            ).start()
        return 0

    lax.fori_loop(0, count, place, 0)

    def drain(g, _):
        flow.finish(g)
        return 0

    lax.fori_loop(0, groups, drain, 0)
    pltpu.make_async_copy(last, last, local_sem.at[0]).wait()


def project(count, tokens, gain, local):
    groups, rows, width = local.shape
    total = tokens.shape[0] * 2
    model = tokens.shape[1]
    vmem = pl.BlockSpec(memory_space=pltpu.VMEM)
    return pl.pallas_call(
        functools.partial(project_kernel, count),
        out_shape=(
            jax.ShapeDtypeStruct((total, width // 2), jnp.bfloat16),
            jax.ShapeDtypeStruct((total, (groups - 2) * width), jnp.bfloat16),
            jax.ShapeDtypeStruct((width, count * rows), jnp.bfloat16),
        ),
        in_specs=[vmem] * 3,
        out_specs=(vmem, vmem, pl.BlockSpec(memory_space=pl.ANY)),
        scratch_shapes=[
            pltpu.VMEM((groups, count, rows, width), jnp.bfloat16),
            pltpu.VMEM((total, model), jnp.bfloat16),
            pltpu.VMEM((total, model), jnp.bfloat16),
            pltpu.SemaphoreType.DMA((groups, 4, 4, count)),
            pltpu.SemaphoreType.DMA((groups, 4, count)),
            pltpu.SemaphoreType.DMA((groups + 1,)),
            pltpu.SemaphoreType.DMA((2,)),
        ],
        compiler_params=pltpu.CompilerParams(
            collective_id=0, has_side_effects=True, vmem_limit_bytes=60 * 1024 * 1024
        ),
        name="project",
    )(tokens, gain.reshape(1, -1), local)


def gather_kernel(count, local, gathered, send_sem, recv_sem, local_sem):
    _, rows, _ = local.shape
    router = Router(count, rows)
    flow = Flow(router, local, gathered, rows, send_sem, recv_sem)
    enter(router, None)
    flow.own(0)
    keep = pltpu.make_async_copy(local.at[0], gathered.at[0, lax.axis_index("sp")], local_sem.at[0])
    keep.start()
    for e in router.events:
        flow.event(0, e)
    keep.wait()
    flow.finish(0)


def gather_small(count, local):
    rows, width = local.shape
    vmem = pl.BlockSpec(memory_space=pltpu.VMEM)
    return pl.pallas_call(
        functools.partial(gather_kernel, count),
        out_shape=jax.ShapeDtypeStruct((1, count, rows, width), local.dtype),
        in_specs=[vmem],
        out_specs=vmem,
        scratch_shapes=[
            pltpu.SemaphoreType.DMA((1, 4, 4, count)),
            pltpu.SemaphoreType.DMA((1, 4, count)),
            pltpu.SemaphoreType.DMA((1,)),
        ],
        compiler_params=pltpu.CompilerParams(collective_id=1, has_side_effects=True),
        name="gather_states",
    )(local[None])[0]


EPSILON = 1e-06
HIGHEST = lax.Precision.HIGHEST


def with_halo(x, sides, width):
    for axis, dim in sides:
        count, length = (lax.axis_size(axis), x.shape[dim])
        up = [(i, (i + 1) % count) for i in range(count - 1)]
        down = [(j, i) for i, j in up]
        last = lax.slice_in_dim(x, length - width, length, axis=dim)
        first = lax.slice_in_dim(x, 0, width, axis=dim)
        before = lax.ppermute(last, axis, up)
        after = lax.ppermute(first, axis, down)
        x = jnp.concatenate([before, x, after], axis=dim)
    return x


def prefix(x, axis, join, neutral, backward):
    count = lax.axis_size(axis)
    place = lax.axis_index(axis)
    ahead = count - 1 - place if backward else place
    gathered = jax.tree.map(
        lambda a, kind: lax.all_gather(a.astype(kind), axis), x, (jnp.bfloat16, jnp.bfloat16)
    )
    state = jax.tree.map(lambda a, e: jnp.zeros_like(a) + jnp.asarray(e, a.dtype), x, neutral)

    def one(step, state):
        source = count - 1 - step if backward else step
        return join(
            state,
            jax.tree.map(
                lambda a, own: lax.dynamic_index_in_dim(a, source, 0, False).astype(own.dtype),
                gathered,
                x,
            ),
        )

    return lax.fori_loop(0, ahead, one, state)


def block_states(scaled_keys, values_block, running):
    closing = running[:, :, -1:]
    totals = jnp.exp(closing[:, :, 0])
    toward_end = jnp.exp(closing - running).transpose(0, 2, 1)[:, :, :, None]
    from_start = jnp.exp(running).transpose(0, 2, 1)[:, :, :, None]
    forward = jnp.einsum(
        "nshd,nshe->nhde", scaled_keys * toward_end, values_block, precision=HIGHEST
    )
    backward = jnp.einsum(
        "nshd,nshe->nhde", scaled_keys * from_start, values_block, precision=HIGHEST
    )
    return (totals, forward, backward)


def block_outputs(queries, scaled_keys, values_block, running, forward_in, backward_in):
    length = queries.shape[1]
    scores = jnp.einsum("nthd,nshd->nhts", queries, scaled_keys, precision=HIGHEST)
    distance = jnp.abs(running[:, :, :, None] - running[:, :, None, :])
    weights = jnp.exp(-distance) + jnp.eye(length, dtype=jnp.float32)
    within = jnp.einsum("nhts,nshe->nthe", scores * weights, values_block, precision=HIGHEST)
    from_start = jnp.exp(running).transpose(0, 2, 1)[:, :, :, None]
    toward_end = jnp.exp(running[:, :, -1:] - running).transpose(0, 2, 1)[:, :, :, None]
    earlier = jnp.einsum("nthd,nhde->nthe", queries, forward_in, precision=HIGHEST)
    after_part = jnp.einsum("nthd,nhde->nthe", queries, backward_in, precision=HIGHEST)
    return within + from_start * earlier + toward_end * after_part


def head_output(retained, gates_in, head_gain):
    row_count = retained.shape[0]
    centred = retained - jnp.mean(retained, axis=2, keepdims=True)
    scaled = centred * lax.rsqrt(jnp.mean(centred * centred, axis=2, keepdims=True) + EPSILON)
    flattened = scaled.reshape(row_count, -1) * head_gain[None, :]
    return (flattened * jax.nn.silu(gates_in.astype(jnp.float32))).astype(jnp.bfloat16)


def normalize(token_block, input_gain):
    widened = token_block.astype(jnp.float32)
    inverse = lax.rsqrt(jnp.mean(widened * widened, axis=1, keepdims=True) + EPSILON)
    return (widened * inverse * input_gain[None, :]).astype(jnp.bfloat16)


def input_mix(products):
    gated_rows = (products[0] * jax.nn.sigmoid(products[1])).astype(jnp.bfloat16)
    others = [member.astype(jnp.bfloat16) for member in products[2:]]
    return jnp.concatenate([gated_rows] + others, axis=1)


def combine_branches(earlier, latter):
    return (earlier[0] * latter[0], latter[0][:, None, None] * earlier[1] + latter[1])


def states_kernel(packed, end_scale, start_scale, forward, backward):
    rows, wide = packed.shape
    width = wide // 4
    pair = 2 * HD
    first = lax.broadcasted_iota(jnp.int32, (rows, pair), 1) < HD
    for h in range(0, width // HD, 2):
        at = h * HD
        keys = packed[:, width + at : width + at + pair].astype(jnp.float32) * HD ** (-0.5)
        values = packed[:, 2 * width + at : 2 * width + at + pair]
        for scale, out in ((end_scale, forward), (start_scale, backward)):
            factor = jnp.where(first, scale[:, h : h + 1], scale[:, h + 1 : h + 2])
            state = lax.dot_general(
                (keys * factor).astype(jnp.bfloat16), values, (((0,), (0,)), ((), ())),
                preferred_element_type=jnp.float32,
            )
            out[0, h] = state[:HD, :HD]
            out[0, h + 1] = state[HD:, HD:]


def fast_states(packed, running):
    blocks, heads, length = running.shape
    closing = running[:, :, -1:]
    end_scale = jnp.exp(closing - running).transpose(0, 2, 1).reshape(-1, heads)
    start_scale = jnp.exp(running).transpose(0, 2, 1).reshape(-1, heads)
    rows = pl.BlockSpec((length, packed.shape[1]), lambda n: (n, 0))
    scale = pl.BlockSpec((length, heads), lambda n: (n, 0))
    state = pl.BlockSpec((1, heads, HD, HD), lambda n: (n, 0, 0, 0))
    shape = jax.ShapeDtypeStruct((blocks, heads, HD, HD), jnp.float32)
    forward, backward = pl.pallas_call(
        states_kernel, grid=(blocks,), in_specs=[rows, scale, scale],
        out_specs=(state, state), out_shape=(shape, shape), name="block_states",
    )(packed, end_scale, start_scale)
    return jnp.exp(closing[:, :, 0]), forward, backward


def retain_kernel(packed, column, row, forward_in, backward_in, gain, out):
    rows, wide = packed.shape
    width = wide // 4
    pair = 2 * HD
    t = lax.broadcasted_iota(jnp.int32, (rows, rows), 0)
    s = lax.broadcasted_iota(jnp.int32, (rows, rows), 1)
    same = jnp.where(t == s, 1.0, 0.0)
    for h in range(0, width // HD, 2):
        at = h * HD
        q, k, v, g = (packed[:, i * width + at : i * width + at + pair] for i in range(4))
        done = []
        for i in range(2):
            lanes = slice(i * HD, (i + 1) * HD)
            head = h + i
            scores = lax.dot_general(
                q[:, lanes], k[:, lanes], (((1,), (1,)), ((), ())),
                preferred_element_type=jnp.float32,
            ) * HD ** (-0.5)
            down = column[:, head : head + 1]
            along = row[0, head : head + 1, :]
            weights = jnp.exp(-jnp.abs(down - along)) + same
            within = jnp.dot(
                (scores * weights).astype(jnp.bfloat16), v[:, lanes],
                preferred_element_type=jnp.float32,
            )
            entering = [
                jnp.dot(q[:, lanes], state[0, head].astype(jnp.bfloat16),
                        preferred_element_type=jnp.float32)
                for state in (forward_in, backward_in)
            ]
            closing = column[rows - 1 : rows, head : head + 1]
            kept = within + jnp.exp(down) * entering[0] + jnp.exp(closing - down) * entering[1]
            centred = kept - jnp.mean(kept, axis=1, keepdims=True)
            done.append(
                centred * lax.rsqrt(jnp.mean(centred * centred, axis=1, keepdims=True) + EPSILON)
            )
        both_heads = jnp.concatenate(done, axis=1) * gain[:, at : at + pair]
        out[:, at : at + pair] = (both_heads * jax.nn.silu(g.astype(jnp.float32))).astype(
            jnp.bfloat16
        )


def fast_retention(packed, running, forward_in, backward_in, head_gain):
    blocks, heads, length = running.shape
    column = running.transpose(0, 2, 1).reshape(-1, heads)
    width = heads * HD
    state = pl.BlockSpec((1, heads, HD, HD), lambda n: (n, 0, 0, 0))
    return pl.pallas_call(
        retain_kernel, grid=(blocks,),
        in_specs=[
            pl.BlockSpec((length, packed.shape[1]), lambda n: (n, 0)),
            pl.BlockSpec((length, heads), lambda n: (n, 0)),
            pl.BlockSpec((1, heads, length), lambda n: (n, 0, 0)),
            state, state,
            pl.BlockSpec((1, width), lambda n: (0, 0)),
        ],
        out_specs=pl.BlockSpec((length, width), lambda n: (n, 0)),
        out_shape=jax.ShapeDtypeStruct((packed.shape[0], width), jnp.bfloat16),
        name="retain",
    )(packed, column, running, forward_in, backward_in, head_gain.reshape(1, -1))


def fits(tokens, weight, output):
    return (
        lax.axis_size("tp") == 2
        and lax.axis_size("sp") % (SIDE * SIDE) == 0
        and weight.shape == (128, 512)
        and output.shape == (512, 128)
        and tokens.shape[0] % 128 == 0
    )


def general_projections(tokens, input_gain, projections):
    group_rows = lax.all_gather(tokens, "tp", axis=0, tiled=True)
    normed = normalize(group_rows, input_gain)
    portions = (
        lax.all_gather(projections[0], "sp", axis=0, tiled=True),
        lax.all_gather(projections[1], "sp", axis=0, tiled=True),
        lax.all_gather(projections[2], "sp", axis=0, tiled=True),
        lax.all_gather(projections[3], "sp", axis=0, tiled=True),
        lax.all_gather(projections[4], "sp", axis=0, tiled=True),
        lax.all_gather(projections[5], "sp", axis=0, tiled=True),
    )
    return input_mix(
        tuple(
            (jnp.dot(normed, portion, preferred_element_type=jnp.float32) for portion in portions)
        )
    )


def fast_prefix(running, forward, backward):
    count = lax.axis_size("sp")
    me = lax.axis_index("sp")
    heads, width = forward.shape[0], forward.shape[1]
    logs = jnp.sum(running[:, :, -1], axis=0)
    coarse = lax.reduce_precision(logs, 8, 7)
    pair = jnp.concatenate([coarse, logs - coarse]).astype(jnp.bfloat16)
    extra = jnp.zeros((16, 128), jnp.bfloat16).at[0, : 2 * heads].set(pair)
    both_states = jnp.stack([forward, backward]).astype(jnp.bfloat16).reshape(-1, 128)
    cut = both_states.shape[0]
    arrived = gather_small(count, jnp.concatenate([both_states, extra], axis=0))
    pair = arrived[:, cut, : 2 * heads].astype(jnp.float32)
    logs = pair[:, :heads] + pair[:, heads:]
    place = jnp.arange(count)
    inner = place[None, :]
    outer = place[:, None]
    left = (inner > outer) & (inner < me)
    right = (inner < outer) & (inner > me)
    left_log = jnp.sum(jnp.where(left[:, :, None], logs[None], 0.0), axis=1)
    right_log = jnp.sum(jnp.where(right[:, :, None], logs[None], 0.0), axis=1)
    left_scale = jnp.where((place < me)[:, None], jnp.exp(left_log), 0.0)
    right_scale = jnp.where((place > me)[:, None], jnp.exp(right_log), 0.0)
    scale = jnp.concatenate([left_scale, right_scale], axis=1)
    scale = jnp.repeat(scale, cut // (2 * heads), axis=1)[:, :, None]
    entering = jnp.sum(scale * arrived[:, :cut].astype(jnp.float32), axis=0)
    enter_left, enter_right = entering.reshape(2, heads, width, width)
    total_left = jnp.exp(jnp.sum(jnp.where((place < me)[:, None], logs, 0.0), axis=0))
    total_right = jnp.exp(jnp.sum(jnp.where((place > me)[:, None], logs, 0.0), axis=0))
    return (total_left, enter_left), (total_right, enter_right)


def body(
    tokens,
    input_gain,
    branch_value,
    branch_gate,
    query_weight,
    key_weight,
    value_weight,
    swish_weight,
    kernel_taps,
    channel_gain,
    decay_logs,
    start_state,
    head_gain,
    output_conv,
    output_heads,
):
    value_width = branch_value.shape[1]
    head_width = query_weight.shape[1]
    fast = fits(tokens, branch_value, output_conv)
    if fast:
        rows = branch_value.shape[0]

        def mixed_columns(a, b):
            return jnp.stack(
                [a.reshape(rows, -1, 128), b.reshape(rows, -1, 128)], axis=2
            ).reshape(rows, -1)

        outputs = jnp.concatenate([output_conv, output_heads], axis=0)
        cut = outputs.shape[1]
        local = jnp.stack(
            [
                mixed_columns(branch_value, branch_gate),
                jnp.concatenate([query_weight, key_weight], axis=1),
                jnp.concatenate([value_weight, swish_weight], axis=1),
                outputs.reshape(-1, cut, cut).transpose(1, 0, 2).reshape(cut, -1),
            ]
        )
        gated_rows, packed, out_weights = project(lax.axis_size("sp"), tokens, input_gain, local)
    else:
        packed = general_projections(
            tokens, input_gain,
            (branch_value, branch_gate, query_weight, key_weight, value_weight, swish_weight),
        )
        gated_rows = packed[:, :value_width]
        packed = packed[:, value_width:]
    row_count = packed.shape[0]
    queries_in = packed[:, :head_width]
    keys_in = packed[:, head_width : 2 * head_width]
    values_in = packed[:, 2 * head_width : 3 * head_width]
    gates_in = packed[:, 3 * head_width :]
    half_width = kernel_taps.shape[0] // 2
    padded = with_halo(gated_rows, (("sp", 0),), half_width).astype(jnp.float32)
    convolved = jnp.zeros((row_count, value_width), jnp.float32)
    for offset in range(kernel_taps.shape[0]):
        convolved = convolved + kernel_taps[offset][None, :] * padded[offset : offset + row_count]
    moments = lax.psum((jnp.sum(convolved, axis=1), jnp.sum(convolved * convolved, axis=1)), "tp")
    average = (moments[0] / DC)[:, None]
    squares = (moments[1] / DC)[:, None]
    normalized = (convolved - average) * lax.rsqrt(squares - average * average + EPSILON)
    branch_out = jax.nn.silu(normalized * channel_gain[None, :]).astype(jnp.bfloat16)
    local_heads = head_width // HD
    blocks = row_count // BLOCK

    def split_heads(matrix):
        return matrix.astype(jnp.float32).reshape(blocks, BLOCK, local_heads, HD)

    query_blocks = split_heads(queries_in)
    key_blocks = split_heads(keys_in) * HD ** (-0.5)
    value_blocks = split_heads(values_in)
    running = jnp.cumsum(decay_logs.reshape(local_heads, blocks, BLOCK).transpose(1, 0, 2), axis=2)
    if fast:
        totals, forward, backward = fast_states(packed, running)
    else:
        totals, forward, backward = block_states(key_blocks, value_blocks, running)
    forward_part = []
    forward_scale = []
    carried = jnp.zeros_like(forward[0])
    factor = jnp.ones_like(totals[0])
    for block_index in range(blocks):
        forward_part.append(carried)
        forward_scale.append(factor)
        carried = totals[block_index][:, None, None] * carried + forward[block_index]
        factor = factor * totals[block_index]
    device_forward = carried
    device_total = factor
    backward_part = [None] * blocks
    reverse_direction_scale = [None] * blocks
    carried = jnp.zeros_like(backward[0])
    factor = jnp.ones_like(totals[0])
    for block_index in reversed(range(blocks)):
        backward_part[block_index] = carried
        reverse_direction_scale[block_index] = factor
        carried = totals[block_index][:, None, None] * carried + backward[block_index]
        factor = factor * totals[block_index]
    identity = (jnp.ones_like(device_total), jnp.zeros_like(device_forward))
    if fast:
        before, after = fast_prefix(running, device_forward, carried)
    else:
        before = prefix((device_total, device_forward), "sp", combine_branches, identity, False)
        after = prefix((device_total, carried), "sp", combine_branches, identity, True)
    enter_forward = before[1] + before[0][:, None, None] * start_state[0]
    enter_backward = after[1] + after[0][:, None, None] * start_state[1]
    forward_in = jnp.stack(
        [
            forward_scale[block_index][:, None, None] * enter_forward + forward_part[block_index]
            for block_index in range(blocks)
        ]
    )
    backward_in = jnp.stack(
        [
            reverse_direction_scale[block_index][:, None, None] * enter_backward
            + backward_part[block_index]
            for block_index in range(blocks)
        ]
    )
    if fast:
        heads_out = fast_retention(packed, running, forward_in, backward_in, head_gain)
    else:
        retained = block_outputs(
            query_blocks, key_blocks, value_blocks, running, forward_in, backward_in
        )
        heads_out = head_output(retained.reshape(row_count, local_heads, HD), gates_in, head_gain)
    if fast:
        partial_sum = jnp.dot(
            jnp.concatenate([branch_out, heads_out], axis=1),
            out_weights,
            preferred_element_type=jnp.float32,
        ).astype(jnp.bfloat16)
        halves = partial_sum.reshape(2, row_count // 2, -1)
        core = lax.axis_index("tp")
        mine = lax.dynamic_index_in_dim(halves, core, 0, False)
        other = lax.dynamic_index_in_dim(halves, 1 - core, 0, False)
        received = lax.ppermute(other, "tp", [(0, 1), (1, 0)])
        return (mine.astype(jnp.float32) + received.astype(jnp.float32)).astype(jnp.bfloat16)
    out_columns = (
        lax.all_gather(output_conv, "sp", axis=1, tiled=True),
        lax.all_gather(output_heads, "sp", axis=1, tiled=True),
    )
    combined = jnp.dot(branch_out, out_columns[0], preferred_element_type=jnp.float32)
    return lax.psum_scatter(
        (combined + jnp.dot(heads_out, out_columns[1], preferred_element_type=jnp.float32)).astype(
            jnp.bfloat16
        ),
        "tp",
        scatter_dimension=0,
        tiled=True,
    )


def solution(mesh):
    in_specs = (
        P(("sp", "tp"), None),
        P(),
        P("sp", "tp"),
        P("sp", "tp"),
        P("sp", "tp"),
        P("sp", "tp"),
        P("sp", "tp"),
        P("sp", "tp"),
        P(None, "tp"),
        P("tp"),
        P("tp", "sp"),
        P(None, "tp", None, None),
        P("tp"),
        P("tp", "sp"),
        P("tp", "sp"),
    )
    out_specs = P(("sp", "tp"), None)
    return jax.shard_map(body, mesh=mesh, in_specs=in_specs, out_specs=out_specs, check_vma=False)
```
